32 devices in a mesh: grp: 2 (over y), fs: 4 (over z), tp: 4 (over x, core).
Axes of the slice: x: 2, y: 2, z: 4, core: 2. Of those that a mesh axis runs over, the one named last changes fastest.
Arguments:
- block_source_tensor: bfloat16 [4096, 2048], P(('grp', 'fs'), 'tp'), parts along dimension 0, may hold values from -6 to 6
- attend_initial_norm_gain: float32 [2048], replicated, may hold values from 0.1 to 1.9
- each_channel_group_norm: float32 [8, 256], P('tp'), may hold values from 0.1 to 1.9
- attend_final_norm_gain: float32 [2048], replicated, may hold values from 0.1 to 1.9
- dense_initial_norm_gain: float32 [2048], replicated, may hold values from 0.1 to 1.9
- dense_final_norm_gain: float32 [2048], replicated, may hold values from 0.1 to 1.9
- question_map: bfloat16 [2048, 1024], P('fs', 'tp'), may hold values from -0.125 to 0.125
- address_map: bfloat16 [2048, 1024], P('fs', 'tp'), may hold values from -0.125 to 0.125
- payload_weights_map: bfloat16 [2048, 2048], P('fs', 'tp'), may hold values from -0.125 to 0.125
- fading_left_factor: bfloat16 [2048, 16], replicated, may hold values from -0.125 to 0.125
- fading_right_factor: float32 [16, 1024], P(None, 'tp'), may hold values from -1.5 to 1.5
- fading_valve_constant: float32 [1024], P('tp'), may hold values from 0.05 to 6.2
- sudden_fade_excess: float32 [4096, 1024], P(('grp', 'fs'), 'tp'), parts along dimension 0, may hold values from -0.7 to 0
- combining_map: bfloat16 [2048, 2048], P('tp', 'fs')
- valve_map: bfloat16 [2048, 3072], P('fs', 'tp'), may hold values from -0.125 to 0.125
- widening_map: bfloat16 [2048, 3072], P('fs', 'tp'), may hold values from -0.125 to 0.125
- valve_conv_stencil: bfloat16 [3, 3072], P(None, 'tp'), may hold values from -3.5 to 3.5
- widening_conv_stencil: bfloat16 [3, 3072], P(None, 'tp'), may hold values from -3.5 to 3.5
- narrowing_map: bfloat16 [3072, 2048], P('tp', 'fs')
Outputs:
- layer_out: bfloat16 [4096, 2048], P(('grp', 'fs'), 'tp'), parts along dimension 0
The draws below stay inside these ranges and needn't reach their ends.
There are 2 independent parts, one for each index of `grp`. The reference program is written for one: setup_inputs(seed, part) draws one part's arguments, and reference() takes and returns one part's arrays. A program takes and returns all parts, laid end to end along the dimension named above; an argument that names none is the same for every part. Nothing has to cross between parts.
All inputs are finite; a program needn't handle non-finite values.
Results may differ from the reference program's by a relative error of at most 0.019.
Values may be sent and summed in bfloat16 or wider, within the bound.
A program may use at most 128 MiB of HBM per device.

```python
import math
import jax
import jax.numpy as jnp
from jax import lax

D = 2048
HEADS = 8
KEY_DIM = 128
VALUE_DIM = 256
FFN_UNITS = 3072
RANK = 16
TAPS = 3
BLOCK = 16
SEQ = 512
TOKENS = 2048
QK_WIDTH = 1024
V_WIDTH = 2048
N_TP = 4


def rising_columns(key, row_count, column_count, ceiling):
    noise_key, jitter_key = jax.random.split(key)
    ramp = ceiling ** (jnp.arange(column_count, dtype=jnp.float32) / column_count)
    jitter = jnp.exp(jax.random.uniform(jitter_key, (column_count,), jnp.float32, -0.35, 0.35))
    noise = jnp.clip(jax.random.normal(noise_key, (row_count, column_count), jnp.float32), -4.0, 4.0)
    return (noise * (ramp * jitter) * row_count ** (-0.5)).astype(jnp.bfloat16)


def draw_combining_map(key, part):
    ceiling = 10.0
    return rising_columns(jax.random.fold_in(key, 11), V_WIDTH, D, ceiling)


def draw_narrowing_map(key, part):
    ceiling = 10.0
    return rising_columns(jax.random.fold_in(key, 23), FFN_UNITS, D, ceiling)


def draw_fading_valve_constant(key, part):
    head_key, slow_key, fast_key = jax.random.split(jax.random.fold_in(key, 37), 3)
    slow_limit = 5
    slow_heads = jax.random.randint(head_key, (HEADS, 1), 0, 10) < slow_limit
    slow_rate = jnp.exp(jax.random.uniform(slow_key, (HEADS, KEY_DIM), jnp.float32, math.log(0.3), math.log(2.0))) / SEQ
    fast_rate = jnp.exp(-jax.random.uniform(fast_key, (HEADS, KEY_DIM), jnp.float32, math.log(30.0), math.log(100.0)))
    step_rate = jnp.where(slow_heads, slow_rate, fast_rate)
    return (-jnp.log(jnp.expm1(16.0 * step_rate))).reshape(QK_WIDTH)


def draw_sudden_fade_excess(key, part):
    spots_key, amount_key = jax.random.split(jax.random.fold_in(key, 53))
    sequences = TOKENS // SEQ
    spots = jax.random.randint(spots_key, (sequences, 3), 0, SEQ)
    struck = jnp.any(jnp.arange(SEQ)[None, None, :] == spots[:, :, None], axis=1)
    amounts = jax.random.uniform(amount_key, (TOKENS, QK_WIDTH), jnp.float32, math.log(0.5), math.log(0.8))
    return jnp.where(struck.reshape(TOKENS, 1), amounts, 0.0)


def block_scale(rng, shape, pieces, least, top_value):
    def one(position, shards_of):
        heights = jax.random.uniform(jax.random.fold_in(jax.random.fold_in(rng, 6), position), (shards_of,), jnp.float32, least / len(pieces), top_value / len(pieces))
        return jnp.repeat(jnp.exp(heights), shape[position] // shards_of).reshape((-1,) + (1,) * (len(shape) - position - 1))

    level = one(*pieces[0])
    for cut in pieces[1:]:
        level = level * one(*cut)
    return level


def normal_values(stream_key, shape, deviation, most, cuts=(), kind=jnp.bfloat16):
    entries = jax.random.normal(stream_key, shape, jnp.float32) * deviation
    if len(cuts) > 0:
        entries = block_scale(stream_key, shape, cuts, -0.22, 0.18) * entries
    return jnp.clip(entries, min=-most, max=most).astype(kind)


def setup_inputs(seed: int = 0, part: int = 0) -> dict:
    key_of = jax.random.split(jax.random.key(seed), 20)
    part_splits = jax.random.split(jax.random.fold_in(key_of[19], part), 20)
    return {
        "block_source_tensor": normal_values(part_splits[0], (TOKENS, D), 1.0, 6.0, ((0, 4), (1, 4))),
        "attend_initial_norm_gain": jnp.clip(1.0 + 0.18 * jax.random.normal(key_of[1], (D,), jnp.float32), 0.1, 1.9),
        "each_channel_group_norm": jnp.clip(1.0 + 0.18 * jax.random.normal(key_of[2], (HEADS, VALUE_DIM), jnp.float32), 0.1, 1.9),
        "attend_final_norm_gain": jnp.clip(1.0 + 0.18 * jax.random.normal(key_of[3], (D,), jnp.float32), 0.1, 1.9),
        "dense_initial_norm_gain": jnp.clip(1.0 + 0.18 * jax.random.normal(key_of[4], (D,), jnp.float32), 0.1, 1.9),
        "dense_final_norm_gain": jnp.clip(1.0 + 0.18 * jax.random.normal(key_of[5], (D,), jnp.float32), 0.1, 1.9),
        "question_map": normal_values(key_of[6], (D, QK_WIDTH), D ** -0.5, 0.125, ((0, 4), (1, 4))),
        "address_map": normal_values(key_of[7], (D, QK_WIDTH), D ** -0.5, 0.125, ((0, 4), (1, 4))),
        "payload_weights_map": normal_values(key_of[8], (D, V_WIDTH), D ** -0.5, 0.125, ((0, 4), (1, 4))),
        "fading_left_factor": normal_values(key_of[9], (D, RANK), D ** -0.5, 0.125),
        "fading_right_factor": normal_values(key_of[10], (RANK, QK_WIDTH), RANK ** -0.5, 1.5, ((1, 4),), jnp.float32),
        "fading_valve_constant": draw_fading_valve_constant(jax.random.fold_in(key_of[19], 71), part),
        "sudden_fade_excess": draw_sudden_fade_excess(jax.random.fold_in(jax.random.fold_in(key_of[19], part), 71), part),
        "combining_map": draw_combining_map(jax.random.fold_in(key_of[19], 71), part),
        "valve_map": normal_values(key_of[14], (D, FFN_UNITS), D ** -0.5, 0.125, ((0, 4), (1, 4))),
        "widening_map": normal_values(key_of[15], (D, FFN_UNITS), D ** -0.5, 0.125, ((0, 4), (1, 4))),
        "valve_conv_stencil": normal_values(key_of[16], (TAPS, FFN_UNITS), TAPS ** -0.5, 3.5, ((1, 4),)),
        "widening_conv_stencil": normal_values(key_of[17], (TAPS, FFN_UNITS), TAPS ** -0.5, 3.5, ((1, 4),)),
        "narrowing_map": draw_narrowing_map(jax.random.fold_in(key_of[19], 71), part),
    }


epsilon = 1e-06
valve_steepness = 16.0
careful_evaluation = lax.Precision.HIGHEST

def norm_rows(values, channel_gain):
    return values * lax.rsqrt(lax.optimization_barrier(jnp.mean(values * values, axis=-1, keepdims=True)) + epsilon) * channel_gain

def rounded(values):
    return lax.optimization_barrier(values.astype(jnp.bfloat16)).astype(jnp.float32)

def gated_linear(query_rows, key_rows, value_rows, fading_typical_span):
    length, head_count, key_width = query_rows.shape
    blocks = length // BLOCK
    query_rows = query_rows.reshape(blocks, BLOCK, head_count, key_width)
    key_rows = key_rows.reshape(blocks, BLOCK, head_count, key_width)
    value_rows = value_rows.reshape(blocks, BLOCK, head_count, -1)
    cumulative = jnp.cumsum(fading_typical_span.reshape(blocks, BLOCK, head_count, key_width), axis=1)
    tail_decay = cumulative[:, -1]
    query_in = query_rows * jnp.exp(cumulative)
    key_in = key_rows * jnp.exp(-cumulative)
    key_end = key_rows * jnp.exp(tail_decay[:, None] - cumulative)
    causal = jnp.tril(jnp.ones((BLOCK, BLOCK), dtype=bool))
    scores = jnp.einsum('nthk,nshk->nhts', query_in, key_in, precision=careful_evaluation)
    scores = jnp.where(causal, scores, 0.0)
    inner = jnp.einsum('nhts,nshv->nthv', scores, value_rows, precision=careful_evaluation)
    states = jnp.einsum('nshk,nshv->nhkv', key_end, value_rows, precision=careful_evaluation)

    def combine(earlier, latter):
        return (earlier[0] * latter[0], latter[0][..., None] * earlier[1] + latter[1])
    running = lax.associative_scan(combine, (jnp.exp(tail_decay), states))[1]
    carried = jnp.concatenate([jnp.zeros_like(running[:1]), running[:-1]], axis=0)
    outer = jnp.einsum('nthk,nhkv->nthv', query_in, carried, precision=careful_evaluation)
    return (inner + outer).reshape(length, head_count, -1)

def causal_taps(values, kernel):
    tap_count = kernel.shape[0]
    length = values.shape[-2]
    padded = jnp.pad(values, [(0, 0)] * (values.ndim - 2) + [(tap_count - 1, 0), (0, 0)])
    kernel = kernel.astype(jnp.float32)
    summed = kernel[0] * padded[..., 0:length, :]
    for offset in range(1, tap_count):
        summed = summed + kernel[offset] * padded[..., offset:offset + length, :]
    return summed

def grouped_sum(left_rows, right_rows, groups):
    span_rows = left_rows.shape[1] // groups
    running_sum = jnp.zeros((left_rows.shape[0], right_rows.shape[1]), jnp.float32)
    for group_index in range(groups):
        low_end = group_index * span_rows
        partial_value = jnp.dot(left_rows[:, low_end:low_end + span_rows], right_rows[low_end:low_end + span_rows], preferred_element_type=jnp.float32)
        running_sum = running_sum + rounded(partial_value)
    return running_sum

def reference(block_source_tensor, attend_initial_norm_gain, each_channel_group_norm, attend_final_norm_gain, dense_initial_norm_gain, dense_final_norm_gain, question_map, address_map, payload_weights_map, fading_left_factor, fading_right_factor, fading_valve_constant, sudden_fade_excess, combining_map, valve_map, widening_map, valve_conv_stencil, widening_conv_stencil, narrowing_map):
    sequences = TOKENS // SEQ
    normed = norm_rows(block_source_tensor.astype(jnp.float32), attend_initial_norm_gain).astype(jnp.bfloat16)
    query_rows = rounded(jnp.dot(normed, question_map, preferred_element_type=jnp.float32)) * KEY_DIM ** (-0.5)
    key_rows = rounded(jnp.dot(normed, address_map, preferred_element_type=jnp.float32))
    value_rows = rounded(jnp.dot(normed, payload_weights_map, preferred_element_type=jnp.float32))
    fading_narrow_count = jnp.dot(normed, fading_left_factor, preferred_element_type=jnp.float32)
    fading_typical_span = jax.nn.log_sigmoid(jnp.dot(fading_narrow_count, fading_right_factor, precision=careful_evaluation) + fading_valve_constant) / valve_steepness + sudden_fade_excess

    def per_sequence(packed):
        return gated_linear(*packed)
    shaped = tuple((member.reshape(sequences, SEQ, HEADS, -1) for member in (query_rows, key_rows, value_rows, fading_typical_span)))
    mixed_heads = lax.map(per_sequence, shaped).reshape(TOKENS, HEADS, VALUE_DIM)
    head_out = norm_rows(mixed_heads, each_channel_group_norm).astype(jnp.bfloat16).reshape(TOKENS, V_WIDTH)
    mixed = grouped_sum(head_out, combining_map, N_TP)
    first = (block_source_tensor.astype(jnp.float32) + norm_rows(mixed, attend_final_norm_gain)).astype(jnp.bfloat16)
    ffn_in = norm_rows(first.astype(jnp.float32), dense_initial_norm_gain).astype(jnp.bfloat16)
    gate_pre = jnp.dot(ffn_in, valve_map, preferred_element_type=jnp.float32).reshape(sequences, SEQ, FFN_UNITS)
    up_pre = jnp.dot(ffn_in, widening_map, preferred_element_type=jnp.float32).reshape(sequences, SEQ, FFN_UNITS)
    hidden = (jax.nn.silu(causal_taps(gate_pre, valve_conv_stencil)) * causal_taps(up_pre, widening_conv_stencil)).astype(jnp.bfloat16)
    channel = grouped_sum(hidden.reshape(TOKENS, FFN_UNITS), narrowing_map, N_TP)
    return (first.astype(jnp.float32) + norm_rows(channel, dense_final_norm_gain)).astype(jnp.bfloat16)
```

```python
import jax
import jax.numpy as jnp
from jax import lax
from jax.experimental import pallas as pl
from jax.experimental.pallas import tpu as pltpu
from jax.sharding import PartitionSpec as P

KEY_DIM = 128
VALUE_DIM = 256
BLOCK = 16


epsilon = 1e-06
valve_steepness = 16.0
careful_evaluation = lax.Precision.HIGHEST


def norm_rows(values, channel_gain):
    return (
        values
        * lax.rsqrt(jnp.mean(values * values, axis=-1, keepdims=True) + epsilon)
        * channel_gain
    )


CHUNK = 64


def contract(left, right, left_dim, right_dim):
    return lax.dot_general(
        left.astype(jnp.bfloat16),
        right.astype(jnp.bfloat16),
        (((left_dim,), (right_dim,)), ((), ())),
        preferred_element_type=jnp.float32,
    )


def mixing_kernel(q_ref, k_ref, v_ref, low_ref, right_ref, valve_ref, excess_ref, gain_ref, out_ref):
    length = q_ref.shape[0]
    head_count = gain_ref.shape[0]
    rows = lax.broadcasted_iota(jnp.int32, (CHUNK, CHUNK), 0)
    columns = lax.broadcasted_iota(jnp.int32, (CHUNK, CHUNK), 1)
    lower = (columns <= rows).astype(jnp.float32)

    def one_chunk(index, states):
        span = pl.ds(pl.multiple_of(index * CHUNK, CHUNK), CHUNK)
        logits = (
            jnp.dot(
                low_ref[span, :],
                right_ref[...],
                precision=careful_evaluation,
                preferred_element_type=jnp.float32,
            )
            + valve_ref[...]
        )
        fading = (
            jnp.minimum(logits, 0.0) - jnp.log1p(jnp.exp(-jnp.abs(logits)))
        ) / valve_steepness + excess_ref[span, :]
        total = jnp.dot(
            lower, fading, precision=careful_evaluation, preferred_element_type=jnp.float32
        )
        after = []
        for head in range(head_count):
            key_span = slice(head * KEY_DIM, (head + 1) * KEY_DIM)
            value_span = slice(head * VALUE_DIM, (head + 1) * VALUE_DIM)
            cum = total[:, key_span]
            query = q_ref[span, key_span].astype(jnp.float32) * KEY_DIM ** (-0.5)
            key = k_ref[span, key_span].astype(jnp.float32)
            value = v_ref[span, value_span]
            state = states[head]
            pieces = []
            for block in range(CHUNK // BLOCK):
                low, high = block * BLOCK, (block + 1) * BLOCK
                start = cum[low - 1 : low] if block else jnp.zeros((1, KEY_DIM), jnp.float32)
                query_in = query[low:high] * jnp.exp(cum[low:high] - start)
                key_in = jnp.concatenate(
                    [key[:high] * jnp.exp(start - cum[:high])]
                    + ([jnp.zeros((CHUNK - high, KEY_DIM), jnp.float32)] if high < CHUNK else []),
                    axis=0,
                )
                pieces.append(contract(query_in, key_in, 1, 1))
            scores = jnp.where(columns <= rows, jnp.concatenate(pieces, axis=0), 0.0)
            tail = cum[CHUNK - 1 :]
            mixed = contract(scores, value, 1, 0) + contract(query * jnp.exp(cum), state, 1, 1)
            after.append(state * jnp.exp(tail) + contract(value, key * jnp.exp(tail - cum), 0, 0))
            out_ref[span, value_span] = norm_rows(mixed, gain_ref[head : head + 1, :]).astype(
                jnp.bfloat16
            )
        return tuple(after)

    empty = tuple(jnp.zeros((VALUE_DIM, KEY_DIM), jnp.float32) for _ in range(head_count))
    lax.fori_loop(0, length // CHUNK, one_chunk, empty, unroll=2)


def mixing(query, key, value, low, right, valve, excess, gain):
    length = query.shape[0]
    flops = length * value.shape[1] * 8 * KEY_DIM
    return pl.pallas_call(
        mixing_kernel,
        out_shape=jax.ShapeDtypeStruct(value.shape, jnp.bfloat16),
        in_specs=[pl.BlockSpec(memory_space=pltpu.VMEM)] * 8,
        out_specs=pl.BlockSpec(memory_space=pltpu.VMEM),
        cost_estimate=pl.CostEstimate(
            flops=60 * flops, bytes_accessed=8 * value.size, transcendentals=0
        ),
    )(query, key, value, low, right, valve, excess, gain)


def causal_taps(values, kernel):
    tap_count = kernel.shape[0]
    length = values.shape[0]
    padded = jnp.pad(values, ((tap_count - 1, 0), (0, 0)))
    kernel = kernel.astype(jnp.float32)
    summed = kernel[0] * padded[0:length]
    for offset in range(1, tap_count):
        summed = summed + kernel[offset] * padded[offset : offset + length]
    return summed


def gather_parts(shard, dimension):
    copies = lax.axis_size("grp")
    part = shard.shape[dimension] // copies
    own = lax.dynamic_slice_in_dim(shard, lax.axis_index("grp") * part, part, axis=dimension)
    return lax.all_gather(own, ("fs", "grp"), axis=dimension, tiled=True)


def on_device(
    block_source_tensor,
    attend_initial_norm_gain,
    each_channel_group_norm,
    attend_final_norm_gain,
    dense_initial_norm_gain,
    dense_final_norm_gain,
    question_map,
    address_map,
    payload_weights_map,
    fading_left_factor,
    fading_right_factor,
    fading_valve_constant,
    sudden_fade_excess,
    combining_map,
    valve_map,
    widening_map,
    valve_conv_stencil,
    widening_conv_stencil,
    narrowing_map,
):
    length, own_columns = block_source_tensor.shape
    tp_index = lax.axis_index("tp")
    full_width = own_columns * lax.axis_size("tp")
    full_rows = lax.all_gather(block_source_tensor, "tp", axis=1, tiled=True)
    normed = norm_rows(full_rows.astype(jnp.float32), attend_initial_norm_gain).astype(jnp.bfloat16)
    qkv_map = gather_parts(
        jnp.concatenate([question_map, address_map, payload_weights_map], axis=1), 0
    )
    qk_columns = question_map.shape[1]
    projected = jnp.dot(normed, qkv_map, preferred_element_type=jnp.float32).astype(jnp.bfloat16)
    low_rank = jnp.dot(normed, fading_left_factor, preferred_element_type=jnp.float32)
    head_out = mixing(
        projected[:, :qk_columns],
        projected[:, qk_columns : 2 * qk_columns],
        projected[:, 2 * qk_columns :],
        low_rank,
        fading_right_factor,
        fading_valve_constant[None],
        sudden_fade_excess,
        each_channel_group_norm,
    )
    partials = jnp.dot(
        head_out,
        gather_parts(combining_map, 1),
        preferred_element_type=jnp.float32,
    )
    mixed = lax.psum_scatter(
        partials.astype(jnp.bfloat16), "tp", scatter_dimension=1, tiled=True
    ).astype(jnp.float32)
    squares = lax.psum(jnp.sum(mixed * mixed, axis=1), "tp")
    own_gain = lax.dynamic_slice_in_dim(attend_final_norm_gain, tp_index * own_columns, own_columns)
    first = (
        block_source_tensor.astype(jnp.float32)
        + mixed * lax.rsqrt(squares / full_width + epsilon)[:, None] * own_gain
    ).astype(jnp.bfloat16)
    first_rows = lax.all_gather(first, "tp", axis=1, tiled=True)
    ffn_in = norm_rows(first_rows.astype(jnp.float32), dense_initial_norm_gain).astype(jnp.bfloat16)

    gate_up_map = gather_parts(jnp.concatenate([valve_map, widening_map], axis=1), 0)
    units = valve_map.shape[1]
    gate_up = jnp.dot(ffn_in, gate_up_map, preferred_element_type=jnp.float32)
    gate_pre, up_pre = gate_up[:, :units], gate_up[:, units:]
    hidden = (
        jax.nn.silu(causal_taps(gate_pre, valve_conv_stencil))
        * causal_taps(up_pre, widening_conv_stencil)
    ).astype(jnp.bfloat16)
    down_partials = jnp.dot(
        hidden,
        gather_parts(narrowing_map, 1),
        preferred_element_type=jnp.float32,
    )
    channel = lax.psum_scatter(
        down_partials.astype(jnp.bfloat16), "tp", scatter_dimension=1, tiled=True
    ).astype(jnp.float32)
    channel_squares = lax.psum(jnp.sum(channel * channel, axis=1), "tp")
    own_post = lax.dynamic_slice_in_dim(dense_final_norm_gain, tp_index * own_columns, own_columns)
    return (
        first.astype(jnp.float32)
        + channel * lax.rsqrt(channel_squares / full_width + epsilon)[:, None] * own_post
    ).astype(jnp.bfloat16)


def solution(mesh):
    placed = (
        P(("grp", "fs"), "tp"),
        P(),
        P("tp", None),
        P(),
        P(),
        P(),
        P("fs", "tp"),
        P("fs", "tp"),
        P("fs", "tp"),
        P(),
        P(None, "tp"),
        P("tp"),
        P(("grp", "fs"), "tp"),
        P("tp", "fs"),
        P("fs", "tp"),
        P("fs", "tp"),
        P(None, "tp"),
        P(None, "tp"),
        P("tp", "fs"),
    )
    return jax.shard_map(
        on_device, mesh=mesh, in_specs=placed, out_specs=P(("grp", "fs"), "tp"), check_vma=False
    )
```

```python
import functools

import jax
import jax.numpy as jnp
from jax import lax
from jax.experimental import pallas as pl
from jax.experimental.pallas import tpu as pltpu
from jax.sharding import PartitionSpec as P

KEY_DIM = 128
VALUE_DIM = 256
BLOCK = 16


epsilon = 1e-06
valve_steepness = 16.0
careful_evaluation = lax.Precision.HIGHEST


def norm_rows(values, channel_gain):
    return (
        values
        * lax.rsqrt(jnp.mean(values * values, axis=-1, keepdims=True) + epsilon)
        * channel_gain
    )


CHUNK = 64


def contract(left, right, left_dim, right_dim):
    return lax.dot_general(
        left.astype(jnp.bfloat16),
        right.astype(jnp.bfloat16),
        (((left_dim,), (right_dim,)), ((), ())),
        preferred_element_type=jnp.float32,
    )


def mixing_kernel(q_ref, k_ref, v_ref, low_ref, right_ref, valve_ref, excess_ref, gain_ref, out_ref):
    length = q_ref.shape[0]
    head_count = gain_ref.shape[0]
    rows = lax.broadcasted_iota(jnp.int32, (CHUNK, CHUNK), 0)
    columns = lax.broadcasted_iota(jnp.int32, (CHUNK, CHUNK), 1)
    lower = (columns <= rows).astype(jnp.float32)

    def one_chunk(index, states):
        span = pl.ds(pl.multiple_of(index * CHUNK, CHUNK), CHUNK)
        logits = (
            jnp.dot(
                low_ref[span, :],
                right_ref[...],
                precision=careful_evaluation,
                preferred_element_type=jnp.float32,
            )
            + valve_ref[...]
        )
        fading = (
            jnp.minimum(logits, 0.0) - jnp.log1p(jnp.exp(-jnp.abs(logits)))
        ) / valve_steepness + excess_ref[span, :]
        total = jnp.dot(
            lower, fading, precision=careful_evaluation, preferred_element_type=jnp.float32
        )
        after = []
        for head in range(head_count):
            key_span = slice(head * KEY_DIM, (head + 1) * KEY_DIM)
            value_span = slice(head * VALUE_DIM, (head + 1) * VALUE_DIM)
            cum = total[:, key_span]
            query = q_ref[span, key_span].astype(jnp.float32) * KEY_DIM ** (-0.5)
            key = k_ref[span, key_span].astype(jnp.float32)
            value = v_ref[span, value_span]
            state = states[head]
            pieces = []
            for block in range(CHUNK // BLOCK):
                low, high = block * BLOCK, (block + 1) * BLOCK
                start = cum[low - 1 : low] if block else jnp.zeros((1, KEY_DIM), jnp.float32)
                query_in = query[low:high] * jnp.exp(cum[low:high] - start)
                key_in = jnp.concatenate(
                    [key[:high] * jnp.exp(start - cum[:high])]
                    + ([jnp.zeros((CHUNK - high, KEY_DIM), jnp.float32)] if high < CHUNK else []),
                    axis=0,
                )
                pieces.append(contract(query_in, key_in, 1, 1))
            scores = jnp.where(columns <= rows, jnp.concatenate(pieces, axis=0), 0.0)
            tail = cum[CHUNK - 1 :]
            mixed = contract(scores, value, 1, 0) + contract(query * jnp.exp(cum), state, 1, 1)
            after.append(state * jnp.exp(tail) + contract(value, key * jnp.exp(tail - cum), 0, 0))
            out_ref[span, value_span] = norm_rows(mixed, gain_ref[head : head + 1, :]).astype(
                jnp.bfloat16
            )
        return tuple(after)

    empty = tuple(jnp.zeros((VALUE_DIM, KEY_DIM), jnp.float32) for _ in range(head_count))
    lax.fori_loop(0, length // CHUNK, one_chunk, empty, unroll=2)


def mixing(query, key, value, low, right, valve, excess, gain):
    length = query.shape[0]
    flops = length * value.shape[1] * 8 * KEY_DIM
    return pl.pallas_call(
        mixing_kernel,
        out_shape=jax.ShapeDtypeStruct(value.shape, jnp.bfloat16),
        in_specs=[pl.BlockSpec(memory_space=pltpu.VMEM)] * 8,
        out_specs=pl.BlockSpec(memory_space=pltpu.VMEM),
        cost_estimate=pl.CostEstimate(
            flops=60 * flops, bytes_accessed=8 * value.size, transcendentals=0
        ),
    )(query, key, value, low, right, valve, excess, gain)


def causal_taps(values, kernel):
    tap_count = kernel.shape[0]
    length = values.shape[0]
    padded = jnp.pad(values, ((tap_count - 1, 0), (0, 0)))
    kernel = kernel.astype(jnp.float32)
    summed = kernel[0] * padded[0:length]
    for offset in range(1, tap_count):
        summed = summed + kernel[offset] * padded[offset : offset + length]
    return summed


MESH = pl.DeviceIdType.MESH


def piece(ref, dimension, owner, part, parts, full):
    if dimension == 0:
        height = ref.shape[0] // (parts * (lax.axis_size("fs") if full else 1))
        first = (owner * parts + part) if full else part
        return ref.at[pl.ds(pl.multiple_of(first * height, height), height), :]
    height = ref.shape[0] // parts
    rows = pl.ds(pl.multiple_of(part * height, height), height)
    if not full:
        return ref.at[rows, :]
    width = ref.shape[1] // lax.axis_size("fs")
    return ref.at[rows, pl.ds(pl.multiple_of(owner * width, width), width)]


def gather_kernel(dimensions, *refs):
    count = len(dimensions)
    shards, maps = refs[:count], refs[count : 2 * count]
    own_sem, line_send, line_recv, part_send, part_recv = refs[2 * count :]
    line, parts = lax.axis_size("fs"), lax.axis_size("grp")
    place, part = lax.axis_index("fs"), lax.axis_index("grp")

    def there(way):
        return place < line - 1 if way == 0 else place > 0

    def toward(way):
        return {"fs": place + 1 if way == 0 else place - 1}

    def part_of(offset):
        return lax.rem(part + offset, parts)

    def line_copy(which, way, step):
        owner = place - step if way == 0 else place + step
        target = piece(maps[which], dimensions[which], owner, part, parts, True)
        return pltpu.make_async_remote_copy(
            src_ref=target,
            dst_ref=target,
            send_sem=line_send.at[which, way, step],
            recv_sem=line_recv.at[which, way, step],
            device_id=toward(way),
            device_id_type=MESH,
        )

    def first_copy(which, way):
        return pltpu.make_async_remote_copy(
            src_ref=piece(shards[which], dimensions[which], place, part, parts, False),
            dst_ref=piece(maps[which], dimensions[which], place, part, parts, True),
            send_sem=line_send.at[which, way, 0],
            recv_sem=line_recv.at[which, way, 0],
            device_id=toward(way),
            device_id_type=MESH,
        )

    def arrival(which, way, step):
        owner = place - step - 1 if way == 0 else place + step + 1
        target = piece(maps[which], dimensions[which], owner, part, parts, True)
        return pltpu.make_async_remote_copy(
            src_ref=target,
            dst_ref=target,
            send_sem=line_send.at[which, way, step],
            recv_sem=line_recv.at[which, way, step],
            device_id=toward(way),
            device_id_type=MESH,
        )

    def part_copy(which, way, step, offset, coming):
        owner = place - step - 1 if way == 0 else place + step + 1
        mine = part_of(parts - offset) if coming else part
        target = piece(maps[which], dimensions[which], owner, mine, parts, True)
        return pltpu.make_async_remote_copy(
            src_ref=target,
            dst_ref=target,
            send_sem=part_send.at[which, way, step, offset - 1],
            recv_sem=part_recv.at[which, way, step, offset - 1],
            device_id={"grp": part_of(offset)},
            device_id_type=MESH,
        )

    def comes(way, step):
        return place - step - 1 >= 0 if way == 0 else place + step + 1 < line

    barrier = pltpu.get_barrier_semaphore()
    for way in range(2):

        @pl.when(there(way))
        def _():
            pl.semaphore_signal(barrier, inc=1, device_id=toward(way), device_id_type=MESH)

    for offset in range(1, parts):
        pl.semaphore_signal(
            barrier, inc=1, device_id={"grp": part_of(offset)}, device_id_type=MESH
        )
    pl.semaphore_wait(
        barrier, there(0).astype(jnp.int32) + there(1).astype(jnp.int32) + parts - 1
    )

    def begin(which):
        for way in range(2):

            @pl.when(there(way))
            def _():
                first_copy(which, way).start()

    def own_copy(which):
        height, width = shards[which].shape
        if dimensions[which] == 0:
            target = maps[which].at[pl.ds(pl.multiple_of(place * height, height), height), :]
        else:
            target = maps[which].at[:, pl.ds(pl.multiple_of(place * width, width), width)]
        return pltpu.make_async_copy(shards[which], target, own_sem.at[which])

    for which in range(min(2, count)):
        begin(which)
    for which in range(count):
        own_copy(which).start()
    for which in range(count):
        if which + 2 < count:
            begin(which + 2)

        @pl.loop(0, line - 1)
        def _(step):
            for way in range(2):

                @pl.when(comes(way, step))
                def _():
                    arrival(which, way, step).wait_recv()

                    @pl.when(there(way))
                    def _():
                        line_copy(which, way, step + 1).start()

                    for offset in range(1, parts):
                        part_copy(which, way, step, offset, False).start()

    for which in range(count):
        own_copy(which).wait()
        for way in range(2):

            @pl.when(there(way))
            def _():
                first_copy(which, way).wait_send()

        @pl.loop(0, line - 1)
        def _(step):
            for way in range(2):

                @pl.when(comes(way, step))
                def _():
                    @pl.when(there(way))
                    def _():
                        line_copy(which, way, step + 1).wait_send()

                    for offset in range(1, parts):
                        part_copy(which, way, step, offset, False).wait_send()
                        part_copy(which, way, step, offset, True).wait_recv()


def gather_maps(shards, dimensions, identity):
    line, parts = lax.axis_size("fs"), lax.axis_size("grp")
    count = len(shards)
    shapes = [
        (shard.shape[0] * line, shard.shape[1]) if dimension == 0 else (shard.shape[0], shard.shape[1] * line)
        for shard, dimension in zip(shards, dimensions)
    ]
    sent = sum(2 * shard.size for shard in shards) * (line - 1)
    return pl.pallas_call(
        functools.partial(gather_kernel, dimensions),
        out_shape=[jax.ShapeDtypeStruct(shape, jnp.bfloat16) for shape in shapes],
        in_specs=[pl.BlockSpec(memory_space=pltpu.VMEM)] * count,
        out_specs=[pl.BlockSpec(memory_space=pl.ANY)] * count,
        scratch_shapes=[
            pltpu.SemaphoreType.DMA((count,)),
            pltpu.SemaphoreType.DMA((count, 2, line)),
            pltpu.SemaphoreType.DMA((count, 2, line)),
            pltpu.SemaphoreType.DMA((count, 2, line, max(parts - 1, 1))),
            pltpu.SemaphoreType.DMA((count, 2, line, max(parts - 1, 1))),
        ],
        compiler_params=pltpu.CompilerParams(collective_id=identity, has_side_effects=True),
        cost_estimate=pl.CostEstimate(flops=0, bytes_accessed=30 * sent, transcendentals=0),
    )(*shards)


def on_device(
    block_source_tensor,
    attend_initial_norm_gain,
    each_channel_group_norm,
    attend_final_norm_gain,
    dense_initial_norm_gain,
    dense_final_norm_gain,
    question_map,
    address_map,
    payload_weights_map,
    fading_left_factor,
    fading_right_factor,
    fading_valve_constant,
    sudden_fade_excess,
    combining_map,
    valve_map,
    widening_map,
    valve_conv_stencil,
    widening_conv_stencil,
    narrowing_map,
):
    length, own_columns = block_source_tensor.shape
    tp_index = lax.axis_index("tp")
    full_width = own_columns * lax.axis_size("tp")
    full_rows = lax.all_gather(block_source_tensor, "tp", axis=1, tiled=True)
    normed = norm_rows(full_rows.astype(jnp.float32), attend_initial_norm_gain).astype(jnp.bfloat16)
    question_full, address_full, payload_full, combining_full = gather_maps(
        (question_map, address_map, payload_weights_map, combining_map), (0, 0, 0, 1), 1
    )
    query, key, value = (
        jnp.dot(normed, full, preferred_element_type=jnp.float32).astype(jnp.bfloat16)
        for full in (question_full, address_full, payload_full)
    )
    low_rank = jnp.dot(normed, fading_left_factor, preferred_element_type=jnp.float32)
    head_out = mixing(
        query,
        key,
        value,
        low_rank,
        fading_right_factor,
        fading_valve_constant[None],
        sudden_fade_excess,
        each_channel_group_norm,
    )
    partials = jnp.dot(
        head_out,
        combining_full,
        preferred_element_type=jnp.float32,
    )
    partials = partials.astype(jnp.bfloat16)
    valve_shard, partials = lax.optimization_barrier((valve_map, partials))
    (valve_full,) = gather_maps((valve_shard,), (0,), 2)
    mixed = lax.psum_scatter(
        partials, "tp", scatter_dimension=1, tiled=True
    )
    mixed, valve_full = lax.optimization_barrier((mixed, valve_full))
    mixed = mixed.astype(jnp.float32)
    squares = lax.psum(jnp.sum(mixed * mixed, axis=1), "tp")
    own_gain = lax.dynamic_slice_in_dim(attend_final_norm_gain, tp_index * own_columns, own_columns)
    first = (
        block_source_tensor.astype(jnp.float32)
        + mixed * lax.rsqrt(squares / full_width + epsilon)[:, None] * own_gain
    ).astype(jnp.bfloat16)
    widening_shard, narrowing_shard, first = lax.optimization_barrier(
        (widening_map, narrowing_map, first)
    )
    widening_full, narrowing_full = gather_maps((widening_shard, narrowing_shard), (0, 1), 3)
    first_rows = lax.all_gather(first, "tp", axis=1, tiled=True)
    ffn_in = norm_rows(first_rows.astype(jnp.float32), dense_initial_norm_gain).astype(jnp.bfloat16)

    gate_pre = jnp.dot(ffn_in, valve_full, preferred_element_type=jnp.float32)
    up_pre = jnp.dot(ffn_in, widening_full, preferred_element_type=jnp.float32)
    hidden = (
        jax.nn.silu(causal_taps(gate_pre, valve_conv_stencil))
        * causal_taps(up_pre, widening_conv_stencil)
    ).astype(jnp.bfloat16)
    down_partials = jnp.dot(
        hidden,
        narrowing_full,
        preferred_element_type=jnp.float32,
    )
    channel = lax.psum_scatter(
        down_partials.astype(jnp.bfloat16), "tp", scatter_dimension=1, tiled=True
    ).astype(jnp.float32)
    channel_squares = lax.psum(jnp.sum(channel * channel, axis=1), "tp")
    own_post = lax.dynamic_slice_in_dim(dense_final_norm_gain, tp_index * own_columns, own_columns)
    return (
        first.astype(jnp.float32)
        + channel * lax.rsqrt(channel_squares / full_width + epsilon)[:, None] * own_post
    ).astype(jnp.bfloat16)


def solution(mesh):
    placed = (
        P(("grp", "fs"), "tp"),
        P(),
        P("tp", None),
        P(),
        P(),
        P(),
        P("fs", "tp"),
        P("fs", "tp"),
        P("fs", "tp"),
        P(),
        P(None, "tp"),
        P("tp"),
        P(("grp", "fs"), "tp"),
        P("tp", "fs"),
        P("fs", "tp"),
        P("fs", "tp"),
        P(None, "tp"),
        P(None, "tp"),
        P("tp", "fs"),
    )
    return jax.shard_map(
        on_device, mesh=mesh, in_specs=placed, out_specs=P(("grp", "fs"), "tp"), check_vma=False
    )
```

```python
import functools

import jax
import jax.numpy as jnp
from jax import lax
from jax.experimental import pallas as pl
from jax.experimental.pallas import tpu as pltpu
from jax.sharding import PartitionSpec as P

KEY_DIM = 128
VALUE_DIM = 256
BLOCK = 16


epsilon = 1e-06
valve_steepness = 16.0
careful_evaluation = lax.Precision.HIGHEST


def norm_rows(values, channel_gain):
    return (
        values
        * lax.rsqrt(jnp.mean(values * values, axis=-1, keepdims=True) + epsilon)
        * channel_gain
    )


CHUNK = 64


def contract(left, right, left_dim, right_dim):
    return lax.dot_general(
        left.astype(jnp.bfloat16),
        right.astype(jnp.bfloat16),
        (((left_dim,), (right_dim,)), ((), ())),
        preferred_element_type=jnp.float32,
    )


def mixing_kernel(q_ref, k_ref, v_ref, low_ref, right_ref, valve_ref, excess_ref, gain_ref, out_ref):
    length = q_ref.shape[0]
    head_count = gain_ref.shape[0]
    rows = lax.broadcasted_iota(jnp.int32, (CHUNK, CHUNK), 0)
    columns = lax.broadcasted_iota(jnp.int32, (CHUNK, CHUNK), 1)
    lower = (columns <= rows).astype(jnp.float32)

    def one_chunk(index, states):
        span = pl.ds(pl.multiple_of(index * CHUNK, CHUNK), CHUNK)
        logits = (
            jnp.dot(
                low_ref[span, :],
                right_ref[...],
                precision=careful_evaluation,
                preferred_element_type=jnp.float32,
            )
            + valve_ref[...]
        )
        fading = (
            jnp.minimum(logits, 0.0) - jnp.log1p(jnp.exp(-jnp.abs(logits)))
        ) / valve_steepness + excess_ref[span, :]
        total = jnp.dot(
            lower, fading, precision=careful_evaluation, preferred_element_type=jnp.float32
        )
        after = []
        for head in range(head_count):
            key_span = slice(head * KEY_DIM, (head + 1) * KEY_DIM)
            value_span = slice(head * VALUE_DIM, (head + 1) * VALUE_DIM)
            cum = total[:, key_span]
            query = q_ref[span, key_span].astype(jnp.float32) * KEY_DIM ** (-0.5)
            key = k_ref[span, key_span].astype(jnp.float32)
            value = v_ref[span, value_span]
            state = states[head]
            pieces = []
            for block in range(CHUNK // BLOCK):
                low, high = block * BLOCK, (block + 1) * BLOCK
                start = cum[low - 1 : low] if block else jnp.zeros((1, KEY_DIM), jnp.float32)
                query_in = query[low:high] * jnp.exp(cum[low:high] - start)
                key_in = jnp.concatenate(
                    [key[:high] * jnp.exp(start - cum[:high])]
                    + ([jnp.zeros((CHUNK - high, KEY_DIM), jnp.float32)] if high < CHUNK else []),
                    axis=0,
                )
                pieces.append(contract(query_in, key_in, 1, 1))
            scores = jnp.where(columns <= rows, jnp.concatenate(pieces, axis=0), 0.0)
            tail = cum[CHUNK - 1 :]
            mixed = contract(scores, value, 1, 0) + contract(query * jnp.exp(cum), state, 1, 1)
            after.append(state * jnp.exp(tail) + contract(value, key * jnp.exp(tail - cum), 0, 0))
            out_ref[span, value_span] = norm_rows(mixed, gain_ref[head : head + 1, :]).astype(
                jnp.bfloat16
            )
        return tuple(after)

    empty = tuple(jnp.zeros((VALUE_DIM, KEY_DIM), jnp.float32) for _ in range(head_count))
    lax.fori_loop(0, length // CHUNK, one_chunk, empty, unroll=2)


def mixing(query, key, value, low, right, valve, excess, gain):
    length = query.shape[0]
    flops = length * value.shape[1] * 8 * KEY_DIM
    return pl.pallas_call(
        mixing_kernel,
        out_shape=jax.ShapeDtypeStruct(value.shape, jnp.bfloat16),
        in_specs=[pl.BlockSpec(memory_space=pltpu.VMEM)] * 8,
        out_specs=pl.BlockSpec(memory_space=pltpu.VMEM),
        cost_estimate=pl.CostEstimate(
            flops=60 * flops, bytes_accessed=8 * value.size, transcendentals=0
        ),
    )(query, key, value, low, right, valve, excess, gain)


def causal_taps(values, kernel):
    tap_count = kernel.shape[0]
    length = values.shape[0]
    padded = jnp.pad(values, ((tap_count - 1, 0), (0, 0)))
    kernel = kernel.astype(jnp.float32)
    summed = kernel[0] * padded[0:length]
    for offset in range(1, tap_count):
        summed = summed + kernel[offset] * padded[offset : offset + length]
    return summed


MESH = pl.DeviceIdType.MESH


def piece(ref, dimension, owner, part, full, cut, cuts):
    parts, line = lax.axis_size("grp"), lax.axis_size("fs")
    height = ref.shape[0] // (parts * cuts * (line if full and dimension == 0 else 1))
    first = part * cuts + cut
    if full and dimension == 0:
        first = owner * parts * cuts + first
    rows = pl.ds(pl.multiple_of(first * height, height), height)
    if not full or dimension == 0:
        return ref.at[rows, :]
    width = ref.shape[1] // line
    return ref.at[rows, pl.ds(pl.multiple_of(owner * width, width), width)]


def cuts_of(shard):
    parts = lax.axis_size("grp")
    cuts = 1
    while shard.size // (parts * 2 * cuts) >= 48 * 1024 and shard.shape[0] % (parts * 2 * cuts * 16) == 0:
        cuts *= 2
    return cuts


def gather_kernel(dimensions, cuts, spread, summed, *refs):
    count = len(dimensions)
    refs = list(refs)

    def take(number):
        taken = refs[:number]
        del refs[:number]
        return taken

    shards, block, partial = take(count), take(spread), take(summed)
    maps, rows_out = take(count), take(spread)
    total_out, squares_out = take(2) if summed else (None, None)
    if count:
        own_sem, line_send, line_recv, part_send, part_recv = take(5)
    if spread:
        spread_own, spread_send, spread_recv = take(3)
    if summed:
        pair_in, chip_sum, chip_in, squares_own, squares_in = take(5)
        pair_send, pair_recv, chip_send, chip_recv, squares_send, squares_recv = take(6)
    ranks, rank = lax.axis_size("tp"), lax.axis_index("tp")
    chips, chip, core = ranks // 2, rank // 2, lax.rem(rank, 2)

    def rank_at(offset):
        return lax.rem(rank + offset, ranks)

    def columns_of(ref, owner):
        width = ref.shape[1] // ranks
        return ref.at[:, pl.ds(pl.multiple_of(owner * width, width), width)]

    def spread_copy(offset, owner):
        return pltpu.make_async_remote_copy(
            src_ref=block[0],
            dst_ref=columns_of(rows_out[0], owner),
            send_sem=spread_send.at[offset],
            recv_sem=spread_recv.at[offset],
            device_id={"tp": rank_at(offset)},
            device_id_type=MESH,
        )

    def spread_local():
        return pltpu.make_async_copy(block[0], columns_of(rows_out[0], rank), spread_own)

    def pair_copy(target):
        return pltpu.make_async_remote_copy(
            src_ref=columns_of(partial[0], target * 2 + 1 - core),
            dst_ref=pair_in.at[target],
            send_sem=pair_send.at[target],
            recv_sem=pair_recv.at[target],
            device_id={"tp": chip * 2 + 1 - core},
            device_id_type=MESH,
        )

    def chip_copy(offset):
        return pltpu.make_async_remote_copy(
            src_ref=chip_sum.at[offset],
            dst_ref=chip_in.at[offset],
            send_sem=chip_send.at[offset],
            recv_sem=chip_recv.at[offset],
            device_id={"tp": lax.rem(chip + offset, chips) * 2 + core},
            device_id_type=MESH,
        )

    def squares_copy(offset):
        return pltpu.make_async_remote_copy(
            src_ref=squares_own,
            dst_ref=squares_in.at[offset],
            send_sem=squares_send.at[offset],
            recv_sem=squares_recv.at[offset],
            device_id={"tp": rank_at(offset)},
            device_id_type=MESH,
        )

    def sum_pairs():
        for target in range(chips):
            pair_copy(target).wait_recv()
        for offset in list(range(1, chips)) + [0]:
            target = lax.rem(chip + offset, chips)
            both = (
                columns_of(partial[0], target * 2 + core)[...].astype(jnp.float32)
                + pair_in[target].astype(jnp.float32)
            )
            if offset:
                chip_sum[offset] = both.astype(jnp.bfloat16)
                chip_copy(offset).start()
            else:
                total_out[...] = both

    def sum_chips():
        for offset in range(1, chips):
            chip_copy(offset).wait_recv()
            total_out[...] += chip_in[offset].astype(jnp.float32)
        total = total_out[...]
        squares_own[...] = lax.dot_general(
            jnp.ones((8, total.shape[1]), jnp.float32),
            total * total,
            (((1,), (1,)), ((), ())),
            precision=careful_evaluation,
            preferred_element_type=jnp.float32,
        )
        for offset in range(1, ranks):
            squares_copy(offset).start()
        summed_squares = squares_own[...]
        for offset in range(1, ranks):
            squares_copy(offset).wait_recv()
            summed_squares = summed_squares + squares_in[offset]
        squares_out[...] = lax.dot_general(
            summed_squares,
            jnp.full((8, 128), 0.125, jnp.float32),
            (((0,), (0,)), ((), ())),
            precision=careful_evaluation,
            preferred_element_type=jnp.float32,
        )
        for target in range(chips):
            pair_copy(target).wait_send()
        for offset in range(1, chips):
            chip_copy(offset).wait_send()
        for offset in range(1, ranks):
            squares_copy(offset).wait_send()

    pieces = [(which, cut) for which in range(count) for cut in range(cuts[which])]
    line, parts = lax.axis_size("fs"), lax.axis_size("grp")
    place, part = lax.axis_index("fs"), lax.axis_index("grp")

    def there(way):
        return place < line - 1 if way == 0 else place > 0

    def toward(way):
        return {"fs": place + 1 if way == 0 else place - 1}

    def part_of(offset):
        return lax.rem(part + offset, parts)

    def at(refs, unit, owner, half, full):
        which, cut = pieces[unit]
        return piece(refs[which], dimensions[which], owner, half, full, cut, cuts[which])

    def line_copy(unit, way, step):
        owner = place - step if way == 0 else place + step
        target = at(maps, unit, owner, part, True)
        return pltpu.make_async_remote_copy(
            src_ref=target,
            dst_ref=target,
            send_sem=line_send.at[unit, way, step],
            recv_sem=line_recv.at[unit, way, step],
            device_id=toward(way),
            device_id_type=MESH,
        )

    def first_copy(unit, way):
        return pltpu.make_async_remote_copy(
            src_ref=at(shards, unit, place, part, False),
            dst_ref=at(maps, unit, place, part, True),
            send_sem=line_send.at[unit, way, 0],
            recv_sem=line_recv.at[unit, way, 0],
            device_id=toward(way),
            device_id_type=MESH,
        )

    def arrival(unit, way, step):
        owner = place - step - 1 if way == 0 else place + step + 1
        target = at(maps, unit, owner, part, True)
        return pltpu.make_async_remote_copy(
            src_ref=target,
            dst_ref=target,
            send_sem=line_send.at[unit, way, step],
            recv_sem=line_recv.at[unit, way, step],
            device_id=toward(way),
            device_id_type=MESH,
        )

    def part_copy(unit, way, step, offset, coming):
        owner = place - step - 1 if way == 0 else place + step + 1
        mine = part_of(parts - offset) if coming else part
        target = at(maps, unit, owner, mine, True)
        return pltpu.make_async_remote_copy(
            src_ref=target,
            dst_ref=target,
            send_sem=part_send.at[unit, way, step, offset - 1],
            recv_sem=part_recv.at[unit, way, step, offset - 1],
            device_id={"grp": part_of(offset)},
            device_id_type=MESH,
        )

    def comes(way, step):
        return place - step - 1 >= 0 if way == 0 else place + step + 1 < line

    barrier = pltpu.get_barrier_semaphore()
    expected = 0
    if count:
        for way in range(2):

            @pl.when(there(way))
            def _():
                pl.semaphore_signal(barrier, inc=1, device_id=toward(way), device_id_type=MESH)

        for offset in range(1, parts):
            pl.semaphore_signal(
                barrier, inc=1, device_id={"grp": part_of(offset)}, device_id_type=MESH
            )
        expected = there(0).astype(jnp.int32) + there(1).astype(jnp.int32) + parts - 1
    if spread or summed:
        for offset in range(1, ranks):
            pl.semaphore_signal(
                barrier, inc=1, device_id={"tp": rank_at(offset)}, device_id_type=MESH
            )
        expected = expected + ranks - 1
    pl.semaphore_wait(barrier, expected)
    if summed:
        for target in range(chips):
            pair_copy(target).start()

    def begin(unit):
        for way in range(2):

            @pl.when(there(way))
            def _():
                first_copy(unit, way).start()

    def own_copy(which):
        height, width = shards[which].shape
        if dimensions[which] == 0:
            target = maps[which].at[pl.ds(pl.multiple_of(place * height, height), height), :]
        else:
            target = maps[which].at[:, pl.ds(pl.multiple_of(place * width, width), width)]
        return pltpu.make_async_copy(shards[which], target, own_sem.at[which])

    def pass_on(unit, step):
        for way in range(2):

            @pl.when(comes(way, step))
            def _():
                arrival(unit, way, step).wait_recv()

                @pl.when(there(way))
                def _():
                    line_copy(unit, way, step + 1).start()

                for offset in range(1, parts):
                    part_copy(unit, way, step, offset, False).start()

    if count:
        begin(0)
    if spread:
        for offset in range(1, ranks):
            spread_copy(offset, rank).start()
        spread_local().start()
    for which in range(count):
        own_copy(which).start()
    if summed:
        sum_pairs()
    for tick in range(len(pieces) + line - 2 if count else 0):
        if tick + 1 < len(pieces):
            begin(tick + 1)
        for step in range(line - 1):
            if 0 <= tick - step < len(pieces):
                pass_on(tick - step, step)

    if summed:
        sum_chips()
    if spread:
        spread_local().wait()
        for offset in range(1, ranks):
            spread_copy(offset, rank).wait_send()
            spread_copy(offset, rank_at(ranks - offset)).wait_recv()
    for which in range(count):
        own_copy(which).wait()
    for unit in range(len(pieces)):
        for way in range(2):

            @pl.when(there(way))
            def _():
                first_copy(unit, way).wait_send()

        @pl.loop(0, line - 1)
        def _(step):
            for way in range(2):

                @pl.when(comes(way, step))
                def _():
                    @pl.when(there(way))
                    def _():
                        line_copy(unit, way, step + 1).wait_send()

                    for offset in range(1, parts):
                        part_copy(unit, way, step, offset, False).wait_send()
                        part_copy(unit, way, step, offset, True).wait_recv()


def exchange(shards, dimensions, identity, block=None, partial=None):
    line, parts, ranks = lax.axis_size("fs"), lax.axis_size("grp"), lax.axis_size("tp")
    count = len(shards)
    cuts = [cuts_of(shard) for shard in shards]
    units = sum(cuts)
    spread, summed = int(block is not None), int(partial is not None)
    vmem, anywhere = pl.BlockSpec(memory_space=pltpu.VMEM), pl.BlockSpec(memory_space=pl.ANY)
    operands = list(shards)
    shapes = [
        jax.ShapeDtypeStruct(
            (shard.shape[0] * line, shard.shape[1])
            if dimension == 0
            else (shard.shape[0], shard.shape[1] * line),
            jnp.bfloat16,
        )
        for shard, dimension in zip(shards, dimensions)
    ]
    out_specs = [anywhere] * count
    scratch = []
    dma = pltpu.SemaphoreType.DMA
    if count:
        scratch += [dma((count,))] + [dma((units, 2, line))] * 2
        scratch += [dma((units, 2, line, max(parts - 1, 1)))] * 2
    if spread:
        operands.append(block)
        shapes.append(jax.ShapeDtypeStruct((block.shape[0], block.shape[1] * ranks), block.dtype))
        out_specs.append(anywhere)
        scratch += [dma] + [dma((ranks,))] * 2
    if summed:
        operands.append(partial)
        length, width = partial.shape[0], partial.shape[1] // ranks
        shapes += [
            jax.ShapeDtypeStruct((length, width), jnp.float32),
            jax.ShapeDtypeStruct((length, 128), jnp.float32),
        ]
        out_specs += [vmem] * 2
        scratch += [pltpu.VMEM((ranks // 2, length, width), jnp.bfloat16)] * 3
        scratch += [pltpu.VMEM((8, length), jnp.float32), pltpu.VMEM((ranks, 8, length), jnp.float32)]
        scratch += [dma((ranks // 2,))] * 4 + [dma((ranks,))] * 2
    return pl.pallas_call(
        functools.partial(gather_kernel, dimensions, cuts, spread, summed),
        out_shape=shapes,
        in_specs=[vmem] * len(operands),
        out_specs=out_specs,
        scratch_shapes=scratch,
        compiler_params=pltpu.CompilerParams(collective_id=identity, has_side_effects=True),
    )(*operands)


def on_device(
    block_source_tensor,
    attend_initial_norm_gain,
    each_channel_group_norm,
    attend_final_norm_gain,
    dense_initial_norm_gain,
    dense_final_norm_gain,
    question_map,
    address_map,
    payload_weights_map,
    fading_left_factor,
    fading_right_factor,
    fading_valve_constant,
    sudden_fade_excess,
    combining_map,
    valve_map,
    widening_map,
    valve_conv_stencil,
    widening_conv_stencil,
    narrowing_map,
):
    length, own_columns = block_source_tensor.shape
    tp_index = lax.axis_index("tp")
    full_width = own_columns * lax.axis_size("tp")
    question_full, address_full, payload_full, combining_full, full_rows = exchange(
        (question_map, address_map, payload_weights_map, combining_map),
        (0, 0, 0, 1),
        1,
        block=block_source_tensor,
    )
    normed = norm_rows(full_rows.astype(jnp.float32), attend_initial_norm_gain).astype(jnp.bfloat16)
    query, key, value = (
        jnp.dot(normed, full, preferred_element_type=jnp.float32).astype(jnp.bfloat16)
        for full in (question_full, address_full, payload_full)
    )
    low_rank = jnp.dot(normed, fading_left_factor, preferred_element_type=jnp.float32)
    head_out = mixing(
        query,
        key,
        value,
        low_rank,
        fading_right_factor,
        fading_valve_constant[None],
        sudden_fade_excess,
        each_channel_group_norm,
    )
    partials = jnp.dot(
        head_out,
        combining_full,
        preferred_element_type=jnp.float32,
    )
    valve_full, mixed, squares = exchange(
        (valve_map,), (0,), 2, partial=partials.astype(jnp.bfloat16)
    )
    own_gain = lax.dynamic_slice_in_dim(attend_final_norm_gain, tp_index * own_columns, own_columns)
    first = (
        block_source_tensor.astype(jnp.float32)
        + mixed * lax.rsqrt(squares[:, :1] / full_width + epsilon) * own_gain
    ).astype(jnp.bfloat16)
    widening_full, narrowing_full, first_rows = exchange(
        (widening_map, narrowing_map), (0, 1), 3, block=first
    )
    ffn_in = norm_rows(first_rows.astype(jnp.float32), dense_initial_norm_gain).astype(jnp.bfloat16)

    gate_pre = jnp.dot(ffn_in, valve_full, preferred_element_type=jnp.float32)
    up_pre = jnp.dot(ffn_in, widening_full, preferred_element_type=jnp.float32)
    hidden = (
        jax.nn.silu(causal_taps(gate_pre, valve_conv_stencil))
        * causal_taps(up_pre, widening_conv_stencil)
    ).astype(jnp.bfloat16)
    down_partials = jnp.dot(
        hidden,
        narrowing_full,
        preferred_element_type=jnp.float32,
    )
    channel, channel_squares = exchange((), (), 4, partial=down_partials.astype(jnp.bfloat16))
    own_post = lax.dynamic_slice_in_dim(dense_final_norm_gain, tp_index * own_columns, own_columns)
    return (
        first.astype(jnp.float32)
        + channel * lax.rsqrt(channel_squares[:, :1] / full_width + epsilon) * own_post
    ).astype(jnp.bfloat16)


def solution(mesh):
    placed = (
        P(("grp", "fs"), "tp"),
        P(),
        P("tp", None),
        P(),
        P(),
        P(),
        P("fs", "tp"),
        P("fs", "tp"),
        P("fs", "tp"),
        P(),
        P(None, "tp"),
        P("tp"),
        P(("grp", "fs"), "tp"),
        P("tp", "fs"),
        P("fs", "tp"),
        P("fs", "tp"),
        P(None, "tp"),
        P(None, "tp"),
        P("tp", "fs"),
    )
    return jax.shard_map(
        on_device, mesh=mesh, in_specs=placed, out_specs=P(("grp", "fs"), "tp"), check_vma=False
    )
```

```python
import functools

import jax
import jax.numpy as jnp
from jax import lax
from jax.experimental import pallas as pl
from jax.experimental.pallas import tpu as pltpu
from jax.sharding import PartitionSpec as P

KEY_DIM = 128
VALUE_DIM = 256
BLOCK = 16


epsilon = 1e-06
valve_steepness = 16.0
careful_evaluation = lax.Precision.HIGHEST


def norm_rows(values, channel_gain):
    return (
        values
        * lax.rsqrt(jnp.mean(values * values, axis=-1, keepdims=True) + epsilon)
        * channel_gain
    )


CHUNK = 64


def contract(left, right, left_dim, right_dim):
    return lax.dot_general(
        left.astype(jnp.bfloat16),
        right.astype(jnp.bfloat16),
        (((left_dim,), (right_dim,)), ((), ())),
        preferred_element_type=jnp.float32,
    )


def mixing_kernel(q_ref, k_ref, v_ref, low_ref, right_ref, valve_ref, excess_ref, gain_ref, out_ref):
    length = q_ref.shape[0]
    head_count = gain_ref.shape[0]
    rows = lax.broadcasted_iota(jnp.int32, (CHUNK, CHUNK), 0)
    columns = lax.broadcasted_iota(jnp.int32, (CHUNK, CHUNK), 1)
    lower = (columns <= rows).astype(jnp.float32)

    def one_chunk(index, states):
        span = pl.ds(pl.multiple_of(index * CHUNK, CHUNK), CHUNK)
        logits = (
            jnp.dot(
                low_ref[span, :],
                right_ref[...],
                precision=careful_evaluation,
                preferred_element_type=jnp.float32,
            )
            + valve_ref[...]
        )
        fading = (
            jnp.minimum(logits, 0.0) - jnp.log1p(jnp.exp(-jnp.abs(logits)))
        ) / valve_steepness + excess_ref[span, :]
        total = jnp.dot(
            lower, fading, precision=careful_evaluation, preferred_element_type=jnp.float32
        )
        after = []
        for head in range(head_count):
            key_span = slice(head * KEY_DIM, (head + 1) * KEY_DIM)
            value_span = slice(head * VALUE_DIM, (head + 1) * VALUE_DIM)
            cum = total[:, key_span]
            query = q_ref[span, key_span].astype(jnp.float32) * KEY_DIM ** (-0.5)
            key = k_ref[span, key_span].astype(jnp.float32)
            value = v_ref[span, value_span]
            state = states[head]
            pieces = []
            for block in range(CHUNK // BLOCK):
                low, high = block * BLOCK, (block + 1) * BLOCK
                start = cum[low - 1 : low] if block else jnp.zeros((1, KEY_DIM), jnp.float32)
                query_in = query[low:high] * jnp.exp(cum[low:high] - start)
                key_in = jnp.concatenate(
                    [key[:high] * jnp.exp(start - cum[:high])]
                    + ([jnp.zeros((CHUNK - high, KEY_DIM), jnp.float32)] if high < CHUNK else []),
                    axis=0,
                )
                pieces.append(contract(query_in, key_in, 1, 1))
            scores = jnp.where(columns <= rows, jnp.concatenate(pieces, axis=0), 0.0)
            tail = cum[CHUNK - 1 :]
            mixed = contract(scores, value, 1, 0) + contract(query * jnp.exp(cum), state, 1, 1)
            after.append(state * jnp.exp(tail) + contract(value, key * jnp.exp(tail - cum), 0, 0))
            out_ref[span, value_span] = norm_rows(mixed, gain_ref[head : head + 1, :]).astype(
                jnp.bfloat16
            )
        return tuple(after)

    empty = tuple(jnp.zeros((VALUE_DIM, KEY_DIM), jnp.float32) for _ in range(head_count))
    lax.fori_loop(0, length // CHUNK, one_chunk, empty, unroll=2)


def mixing(query, key, value, low, right, valve, excess, gain):
    length = query.shape[0]
    flops = length * value.shape[1] * 8 * KEY_DIM
    return pl.pallas_call(
        mixing_kernel,
        out_shape=jax.ShapeDtypeStruct(value.shape, jnp.bfloat16),
        in_specs=[pl.BlockSpec(memory_space=pltpu.VMEM)] * 8,
        out_specs=pl.BlockSpec(memory_space=pltpu.VMEM),
        cost_estimate=pl.CostEstimate(
            flops=60 * flops, bytes_accessed=8 * value.size, transcendentals=0
        ),
    )(query, key, value, low, right, valve, excess, gain)


def causal_taps(values, kernel):
    tap_count = kernel.shape[0]
    length = values.shape[0]
    padded = jnp.pad(values, ((tap_count - 1, 0), (0, 0)))
    kernel = kernel.astype(jnp.float32)
    summed = kernel[0] * padded[0:length]
    for offset in range(1, tap_count):
        summed = summed + kernel[offset] * padded[offset : offset + length]
    return summed


MESH = pl.DeviceIdType.MESH


def piece(ref, dimension, owner, part, full, cut, cuts):
    parts, line = lax.axis_size("grp"), lax.axis_size("fs")
    height = ref.shape[0] // (parts * cuts * (line if full and dimension == 0 else 1))
    first = part * cuts + cut
    if full and dimension == 0:
        first = owner * parts * cuts + first
    rows = pl.ds(pl.multiple_of(first * height, height), height)
    if not full or dimension == 0:
        return ref.at[rows, :]
    width = ref.shape[1] // line
    return ref.at[rows, pl.ds(pl.multiple_of(owner * width, width), width)]


def cuts_of(shard):
    parts = lax.axis_size("grp")
    cuts = 1
    while shard.size // (parts * 2 * cuts) >= 48 * 1024 and shard.shape[0] % (parts * 2 * cuts * 16) == 0:
        cuts *= 2
    return cuts


def gather_kernel(dimensions, cuts, spread, summed, *refs):
    count = len(dimensions)
    refs = list(refs)

    def take(number):
        taken = refs[:number]
        del refs[:number]
        return taken

    shards, block, partial = take(count), take(spread), take(summed)
    maps, rows_out = take(count), take(spread)
    total_out, squares_out = take(2) if summed else (None, None)
    if count:
        own_sem, line_send, line_recv, part_send, part_recv = take(5)
    if spread:
        spread_own, spread_send, spread_recv = take(3)
    if summed:
        pair_in, chip_sum, chip_in, squares_own, squares_in = take(5)
        pair_send, pair_recv, chip_send, chip_recv, squares_send, squares_recv = take(6)
    ranks, rank = lax.axis_size("tp"), lax.axis_index("tp")
    chips, chip, core = ranks // 2, rank // 2, lax.rem(rank, 2)

    def rank_at(offset):
        return lax.rem(rank + offset, ranks)

    def columns_of(ref, owner):
        width = ref.shape[1] // ranks
        return ref.at[:, pl.ds(pl.multiple_of(owner * width, width), width)]

    def spread_copy(offset, owner):
        return pltpu.make_async_remote_copy(
            src_ref=block[0],
            dst_ref=columns_of(rows_out[0], owner),
            send_sem=spread_send.at[offset],
            recv_sem=spread_recv.at[offset],
            device_id={"tp": rank_at(offset)},
            device_id_type=MESH,
        )

    def spread_local():
        return pltpu.make_async_copy(block[0], columns_of(rows_out[0], rank), spread_own)

    def pair_copy(target):
        return pltpu.make_async_remote_copy(
            src_ref=columns_of(partial[0], target * 2 + 1 - core),
            dst_ref=pair_in.at[target],
            send_sem=pair_send.at[target],
            recv_sem=pair_recv.at[target],
            device_id={"tp": chip * 2 + 1 - core},
            device_id_type=MESH,
        )

    def chip_copy(offset):
        return pltpu.make_async_remote_copy(
            src_ref=chip_sum.at[offset],
            dst_ref=chip_in.at[offset],
            send_sem=chip_send.at[offset],
            recv_sem=chip_recv.at[offset],
            device_id={"tp": lax.rem(chip + offset, chips) * 2 + core},
            device_id_type=MESH,
        )

    def squares_copy(offset):
        return pltpu.make_async_remote_copy(
            src_ref=squares_own,
            dst_ref=squares_in.at[offset],
            send_sem=squares_send.at[offset],
            recv_sem=squares_recv.at[offset],
            device_id={"tp": rank_at(offset)},
            device_id_type=MESH,
        )

    def sum_pairs():
        for target in range(chips):
            pair_copy(target).wait_recv()
        for offset in list(range(1, chips)) + [0]:
            target = lax.rem(chip + offset, chips)
            both = (
                columns_of(partial[0], target * 2 + core)[...].astype(jnp.float32)
                + pair_in[target].astype(jnp.float32)
            )
            if offset:
                chip_sum[offset] = both.astype(jnp.bfloat16)
                chip_copy(offset).start()
            else:
                total_out[...] = both

    def sum_chips():
        for offset in range(1, chips):
            chip_copy(offset).wait_recv()
            total_out[...] += chip_in[offset].astype(jnp.float32)
        total = total_out[...]
        squares_own[...] = lax.dot_general(
            jnp.ones((8, total.shape[1]), jnp.float32),
            total * total,
            (((1,), (1,)), ((), ())),
            precision=careful_evaluation,
            preferred_element_type=jnp.float32,
        )
        for offset in range(1, ranks):
            squares_copy(offset).start()
        summed_squares = squares_own[...]
        for offset in range(1, ranks):
            squares_copy(offset).wait_recv()
            summed_squares = summed_squares + squares_in[offset]
        squares_out[...] = lax.dot_general(
            summed_squares,
            jnp.full((8, 128), 0.125, jnp.float32),
            (((0,), (0,)), ((), ())),
            precision=careful_evaluation,
            preferred_element_type=jnp.float32,
        )
        for target in range(chips):
            pair_copy(target).wait_send()
        for offset in range(1, chips):
            chip_copy(offset).wait_send()
        for offset in range(1, ranks):
            squares_copy(offset).wait_send()

    pieces = [(which, cut) for which in range(count) for cut in range(cuts[which])]
    line, parts = lax.axis_size("fs"), lax.axis_size("grp")
    place, part = lax.axis_index("fs"), lax.axis_index("grp")

    def there(way):
        return place < line - 1 if way == 0 else place > 0

    def toward(way):
        return {"fs": place + 1 if way == 0 else place - 1}

    def part_of(offset):
        return lax.rem(part + offset, parts)

    def at(refs, unit, owner, half, full):
        which, cut = pieces[unit]
        return piece(refs[which], dimensions[which], owner, half, full, cut, cuts[which])

    def line_copy(unit, way, step):
        owner = place - step if way == 0 else place + step
        target = at(maps, unit, owner, part, True)
        return pltpu.make_async_remote_copy(
            src_ref=target,
            dst_ref=target,
            send_sem=line_send.at[unit, way, step],
            recv_sem=line_recv.at[unit, way, step],
            device_id=toward(way),
            device_id_type=MESH,
        )

    def first_copy(unit, way):
        return pltpu.make_async_remote_copy(
            src_ref=at(shards, unit, place, part, False),
            dst_ref=at(maps, unit, place, part, True),
            send_sem=line_send.at[unit, way, 0],
            recv_sem=line_recv.at[unit, way, 0],
            device_id=toward(way),
            device_id_type=MESH,
        )

    def arrival(unit, way, step):
        owner = place - step - 1 if way == 0 else place + step + 1
        target = at(maps, unit, owner, part, True)
        return pltpu.make_async_remote_copy(
            src_ref=target,
            dst_ref=target,
            send_sem=line_send.at[unit, way, step],
            recv_sem=line_recv.at[unit, way, step],
            device_id=toward(way),
            device_id_type=MESH,
        )

    def part_copy(unit, way, step, offset, coming):
        owner = place - step - 1 if way == 0 else place + step + 1
        mine = part_of(parts - offset) if coming else part
        target = at(maps, unit, owner, mine, True)
        return pltpu.make_async_remote_copy(
            src_ref=target,
            dst_ref=target,
            send_sem=part_send.at[unit, way, step, offset - 1],
            recv_sem=part_recv.at[unit, way, step, offset - 1],
            device_id={"grp": part_of(offset)},
            device_id_type=MESH,
        )

    def comes(way, step):
        return place - step - 1 >= 0 if way == 0 else place + step + 1 < line

    barrier = pltpu.get_barrier_semaphore()
    expected = 0
    if count:
        for way in range(2):

            @pl.when(there(way))
            def _():
                pl.semaphore_signal(barrier, inc=1, device_id=toward(way), device_id_type=MESH)

        for offset in range(1, parts):
            pl.semaphore_signal(
                barrier, inc=1, device_id={"grp": part_of(offset)}, device_id_type=MESH
            )
        expected = there(0).astype(jnp.int32) + there(1).astype(jnp.int32) + parts - 1
    if spread or summed:
        for offset in range(1, ranks):
            pl.semaphore_signal(
                barrier, inc=1, device_id={"tp": rank_at(offset)}, device_id_type=MESH
            )
        expected = expected + ranks - 1
    pl.semaphore_wait(barrier, expected)
    if summed:
        for target in range(chips):
            pair_copy(target).start()

    def begin(unit):
        for way in range(2):

            @pl.when(there(way))
            def _():
                first_copy(unit, way).start()

    def own_copy(which):
        height, width = shards[which].shape
        if dimensions[which] == 0:
            target = maps[which].at[pl.ds(pl.multiple_of(place * height, height), height), :]
        else:
            target = maps[which].at[:, pl.ds(pl.multiple_of(place * width, width), width)]
        return pltpu.make_async_copy(shards[which], target, own_sem.at[which])

    def pass_on(unit, step):
        for way in range(2):

            @pl.when(comes(way, step))
            def _():
                arrival(unit, way, step).wait_recv()

                @pl.when(there(way))
                def _():
                    line_copy(unit, way, step + 1).start()

                for offset in range(1, parts):
                    part_copy(unit, way, step, offset, False).start()

    if count:
        begin(0)
    if spread:
        for offset in range(1, ranks):
            spread_copy(offset, rank).start()
        spread_local().start()
    for which in range(count):
        own_copy(which).start()
    if summed:
        sum_pairs()
    for tick in range(len(pieces) + line - 2 if count else 0):
        if tick + 1 < len(pieces):
            begin(tick + 1)
        for step in range(line - 1):
            if 0 <= tick - step < len(pieces):
                pass_on(tick - step, step)

    if summed:
        sum_chips()
    if spread:
        spread_local().wait()
        for offset in range(1, ranks):
            spread_copy(offset, rank).wait_send()
            spread_copy(offset, rank_at(ranks - offset)).wait_recv()
    for which in range(count):
        own_copy(which).wait()
    for unit in range(len(pieces)):
        for way in range(2):

            @pl.when(there(way))
            def _():
                first_copy(unit, way).wait_send()

        @pl.loop(0, line - 1)
        def _(step):
            for way in range(2):

                @pl.when(comes(way, step))
                def _():
                    @pl.when(there(way))
                    def _():
                        line_copy(unit, way, step + 1).wait_send()

                    for offset in range(1, parts):
                        part_copy(unit, way, step, offset, False).wait_send()
                        part_copy(unit, way, step, offset, True).wait_recv()


def exchange(shards, dimensions, identity, block=None, partial=None):
    line, parts, ranks = lax.axis_size("fs"), lax.axis_size("grp"), lax.axis_size("tp")
    count = len(shards)
    cuts = [cuts_of(shard) for shard in shards]
    units = sum(cuts)
    spread, summed = int(block is not None), int(partial is not None)
    vmem = pl.BlockSpec(memory_space=pltpu.VMEM)
    operands = list(shards)
    shapes = [
        jax.ShapeDtypeStruct(
            (shard.shape[0] * line, shard.shape[1])
            if dimension == 0
            else (shard.shape[0], shard.shape[1] * line),
            jnp.bfloat16,
        )
        for shard, dimension in zip(shards, dimensions)
    ]
    out_specs = [vmem] * count
    scratch = []
    dma = pltpu.SemaphoreType.DMA
    if count:
        scratch += [dma((count,))] + [dma((units, 2, line))] * 2
        scratch += [dma((units, 2, line, max(parts - 1, 1)))] * 2
    if spread:
        operands.append(block)
        shapes.append(jax.ShapeDtypeStruct((block.shape[0], block.shape[1] * ranks), block.dtype))
        out_specs.append(vmem)
        scratch += [dma] + [dma((ranks,))] * 2
    if summed:
        operands.append(partial)
        length, width = partial.shape[0], partial.shape[1] // ranks
        shapes += [
            jax.ShapeDtypeStruct((length, width), jnp.float32),
            jax.ShapeDtypeStruct((length, 128), jnp.float32),
        ]
        out_specs += [vmem] * 2
        scratch += [pltpu.VMEM((ranks // 2, length, width), jnp.bfloat16)] * 3
        scratch += [pltpu.VMEM((8, length), jnp.float32), pltpu.VMEM((ranks, 8, length), jnp.float32)]
        scratch += [dma((ranks // 2,))] * 4 + [dma((ranks,))] * 2
    return pl.pallas_call(
        functools.partial(gather_kernel, dimensions, cuts, spread, summed),
        out_shape=shapes,
        in_specs=[vmem] * len(operands),
        out_specs=out_specs,
        scratch_shapes=scratch,
        compiler_params=pltpu.CompilerParams(collective_id=identity, has_side_effects=True),
    )(*operands)


def on_device(
    block_source_tensor,
    attend_initial_norm_gain,
    each_channel_group_norm,
    attend_final_norm_gain,
    dense_initial_norm_gain,
    dense_final_norm_gain,
    question_map,
    address_map,
    payload_weights_map,
    fading_left_factor,
    fading_right_factor,
    fading_valve_constant,
    sudden_fade_excess,
    combining_map,
    valve_map,
    widening_map,
    valve_conv_stencil,
    widening_conv_stencil,
    narrowing_map,
):
    length, own_columns = block_source_tensor.shape
    tp_index = lax.axis_index("tp")
    full_width = own_columns * lax.axis_size("tp")
    question_full, address_full, payload_full, combining_full, full_rows = exchange(
        (question_map, address_map, payload_weights_map, combining_map),
        (0, 0, 0, 1),
        1,
        block=block_source_tensor,
    )
    normed = norm_rows(full_rows.astype(jnp.float32), attend_initial_norm_gain).astype(jnp.bfloat16)
    query, key, value = (
        jnp.dot(normed, full, preferred_element_type=jnp.float32).astype(jnp.bfloat16)
        for full in (question_full, address_full, payload_full)
    )
    low_rank = jnp.dot(normed, fading_left_factor, preferred_element_type=jnp.float32)
    head_out = mixing(
        query,
        key,
        value,
        low_rank,
        fading_right_factor,
        fading_valve_constant[None],
        sudden_fade_excess,
        each_channel_group_norm,
    )
    partials = jnp.dot(
        head_out,
        combining_full,
        preferred_element_type=jnp.float32,
    )
    valve_full, mixed, squares = exchange(
        (valve_map,), (0,), 2, partial=partials.astype(jnp.bfloat16)
    )
    own_gain = lax.dynamic_slice_in_dim(attend_final_norm_gain, tp_index * own_columns, own_columns)
    first = (
        block_source_tensor.astype(jnp.float32)
        + mixed * lax.rsqrt(squares[:, :1] / full_width + epsilon) * own_gain
    ).astype(jnp.bfloat16)
    widening_full, narrowing_full, first_rows = exchange(
        (widening_map, narrowing_map), (0, 1), 3, block=first
    )
    ffn_in = norm_rows(first_rows.astype(jnp.float32), dense_initial_norm_gain).astype(jnp.bfloat16)

    gate_pre = jnp.dot(ffn_in, valve_full, preferred_element_type=jnp.float32)
    up_pre = jnp.dot(ffn_in, widening_full, preferred_element_type=jnp.float32)
    hidden = (
        jax.nn.silu(causal_taps(gate_pre, valve_conv_stencil))
        * causal_taps(up_pre, widening_conv_stencil)
    ).astype(jnp.bfloat16)
    down_partials = jnp.dot(
        hidden,
        narrowing_full,
        preferred_element_type=jnp.float32,
    )
    channel, channel_squares = exchange((), (), 4, partial=down_partials.astype(jnp.bfloat16))
    own_post = lax.dynamic_slice_in_dim(dense_final_norm_gain, tp_index * own_columns, own_columns)
    return (
        first.astype(jnp.float32)
        + channel * lax.rsqrt(channel_squares[:, :1] / full_width + epsilon) * own_post
    ).astype(jnp.bfloat16)


def solution(mesh):
    placed = (
        P(("grp", "fs"), "tp"),
        P(),
        P("tp", None),
        P(),
        P(),
        P(),
        P("fs", "tp"),
        P("fs", "tp"),
        P("fs", "tp"),
        P(),
        P(None, "tp"),
        P("tp"),
        P(("grp", "fs"), "tp"),
        P("tp", "fs"),
        P("fs", "tp"),
        P("fs", "tp"),
        P(None, "tp"),
        P(None, "tp"),
        P("tp", "fs"),
    )
    return jax.shard_map(
        on_device, mesh=mesh, in_specs=placed, out_specs=P(("grp", "fs"), "tp"), check_vma=False
    )
```
